32 devices in a mesh: sp: 16 (over z, y, x), tp: 2 (over core).
Axes of the slice: x: 2, y: 2, z: 4, core: 2. Of those that a mesh axis runs over, the one named last changes fastest.
Arguments:
- residual: bfloat16 [4096, 2048], P(('sp', 'tp')), may hold values from -6 to 6
- query_one: bfloat16 [4096, 512], P('sp', 'tp'), may hold values from -6.5 to 6.5
- key_one: bfloat16 [4096, 512], P('sp', 'tp'), may hold values from -6.5 to 6.5
- query_two: bfloat16 [4096, 512], P('sp', 'tp'), may hold values from -6.5 to 6.5
- key_two: bfloat16 [4096, 512], P('sp', 'tp'), may hold values from -6.5 to 6.5
- value_rows: bfloat16 [4096, 1024], P('sp', 'tp'), may hold values from -6 to 6
- lambda_head: float32 [8], P('tp'), may hold values from 0.3 to 0.8
- head_gain: float32 [128], replicated, may hold values from 0.1 to 1.9
- out_weight: bfloat16 [1024, 2048], replicated, may hold values from -0.1875 to 0.1875
- norm_gain: float32 [2048], replicated, may hold values from 0.1 to 1.9
- route_ids: int32 [4096, 2], P(('sp', 'tp')), may hold values from 0 to 15, all different within a row; in each aligned block of 128 rows (0 to 127, 128 to 255, ...) at most 24 rows name the same one
- route_weights: float32 [4096, 2], P(('sp', 'tp')), may hold values from 0.25 to 1
- gate_weight: bfloat16 [16, 2048, 512], P('sp', None, 'tp'), may hold values from -0.125 to 0.125
- up_weight: bfloat16 [16, 2048, 512], P('sp', None, 'tp'), may hold values from -0.125 to 0.125
- down_weight: bfloat16 [16, 512, 2048], P('sp', 'tp'), may hold values from -0.25 to 0.25
Outputs:
- mixed: bfloat16 [4096, 2048], P(('sp', 'tp'))
The draws below stay inside these ranges and needn't reach their ends.
Inputs may be any that keep to these rules, and one draw needn't show every extreme that they name: `route_ids`: each row names 2 different experts. Among the rows of one device (aligned blocks of 128 rows) no expert is named more than 24 times, and in every draw some device has an expert named exactly 24 times.
All inputs are finite; a program needn't handle non-finite values.
Results may differ from the reference program's by a relative error of at most 0.014.
Values may be sent and summed in bfloat16 or wider, within the bound.
A program may use at most 128 MiB of HBM per device.

```python
import math
import jax
import jax.numpy as jnp
import numpy as np
from jax import lax

D = 2048
HEADS = 8
HD = 64
VD = 128
FF = 512
TOPK = 2
TOK_DEV = 256
TOKENS = 4096
EXPERTS = 16
CAP = 24
N_SP = 16
N_TP = 2


def draw_queries(key, map_index):
    sample = 1.3 * jax.random.normal(jax.random.fold_in(key, 11 + map_index), (TOKENS, HEADS * HD), jnp.float32)
    sample = jnp.clip(sample, -6.5, 6.5)
    return sample.astype(jnp.bfloat16)


def draw_keys(key, map_index):
    sample = 1.3 * jax.random.normal(jax.random.fold_in(key, 21 + map_index), (TOKENS, HEADS * HD), jnp.float32)
    sample = jnp.clip(sample, -6.5, 6.5)
    return sample.astype(jnp.bfloat16)


def draw_query_one(key, part):
    return draw_queries(key, 0)


def draw_key_one(key, part):
    return draw_keys(key, 0)


def draw_query_two(key, part):
    return draw_queries(key, 1)


def draw_key_two(key, part):
    return draw_keys(key, 1)


def levels(key, dims, shards, least, high):
    gain = 1.0
    for dim, blocks in shards:
        heights = jax.random.uniform(jax.random.fold_in(jax.random.fold_in(key, 6), dim), (blocks,), jnp.float32, least / len(shards), high / len(shards))
        gain = gain * jnp.repeat(jnp.exp(heights), dims[dim] // blocks).reshape((-1,) + (1,) * (len(dims) - 1 - dim))
    return gain


def routed_block(rng, own, number, rows, number_of, top, limit, skew):
    order = jax.random.permutation(rng, number_of)
    packed, ordinary = shares(number_of, rows * top, limit, skew, True), shares(number_of, rows * top, limit, skew, False)
    places = jnp.arange(number_of)

    def named(lengths, turn):
        used = int((lengths > 0).sum())
        fixed = max(1, used // 4)
        shifted = fixed + (places - fixed + turn * (used - fixed)) % max(1, number_of - fixed)
        return jnp.zeros((number_of,), jnp.int32).at[order[jnp.where(places < fixed, places, shifted)]].set(jnp.asarray(lengths, jnp.int32))

    lengths = jnp.where(number % 4 == 0, named(packed, number // 4), named(ordinary, number - number // 4 - 1))
    mixed = jax.random.permutation(jax.random.fold_in(own, 3), number_of)
    giver, taker = mixed[0:number_of // 2 * 2:2], mixed[1:number_of // 2 * 2:2]
    margin = jnp.minimum(lengths[giver] - 1, limit - lengths[taker]) // 2
    margin = jnp.where((giver == order[0]) | (taker == order[0]) | (lengths[taker] == 0), 0, jnp.maximum(margin, 0))
    shifted = jax.random.randint(jax.random.fold_in(own, 4), (number_of // 2,), 0, 1 << 20) % (margin + 1)
    lengths = lengths.at[giver].add(-shifted).at[taker].add(shifted)
    members = jnp.searchsorted(jnp.cumsum(lengths), jnp.arange(rows * top), side="right").astype(jnp.int32)
    grid = members.reshape(top, rows).T
    grid = grid[jax.random.permutation(jax.random.fold_in(own, 1), rows)]
    turn = jax.random.randint(jax.random.fold_in(own, 2), (rows, 1), 0, top)
    return jnp.take_along_axis(grid, (jnp.arange(top)[None, :] + turn) % top, axis=1)


def shares(amount, total, bound, lean, full):
    loads = [(1 << 20) // math.isqrt(standing ** lean) + 1 for standing in range(1, amount + 1)]
    largest = bound if full else min(bound, max(-(-total // amount), total * loads[0] // sum(loads)))
    least = 1 if total - largest >= amount - 1 else 0
    holding, spare = [largest] + [least] * (amount - 1), total - largest - least * (amount - 1)
    while spare > 0:
        candidates = [i for i in range(1, amount) if holding[i] < largest] or [i for i in range(1, amount) if holding[i] < bound]
        whole, budget = sum([loads[i] for i in candidates]), spare
        for i in candidates:
            more = min(bound - holding[i], max(1, budget * loads[i] // whole), spare)
            holding[i] = holding[i] + more
            spare = spare - more
    return np.array(holding)


def normal_values(own_key, dims, width, most, pieces=(), kind=jnp.bfloat16):
    level = levels(own_key, dims, pieces, -0.22, 0.18) if pieces else 1.0
    values = jax.random.normal(own_key, dims, jnp.float32) * width * level
    return jnp.minimum(jnp.maximum(values, -most), most).astype(kind)


def setup_inputs(seed: int = 0) -> dict:
    seeds = jax.random.split(jax.random.key(seed), 16)
    residual = normal_values(seeds[0], (TOKENS, D), 1.0, 6.0, ((0, 32),))
    query_one = draw_query_one(jax.random.fold_in(seeds[15], 71), 0)
    key_one = draw_key_one(jax.random.fold_in(seeds[15], 71), 0)
    query_two = draw_query_two(jax.random.fold_in(seeds[15], 71), 0)
    key_two = draw_key_two(jax.random.fold_in(seeds[15], 71), 0)
    value_rows = normal_values(seeds[5], (TOKENS, HEADS * VD), 1.0, 6.0, ((0, 16), (1, 2)))
    lambda_head = jnp.clip(0.3 + 0.5 * jax.random.uniform(seeds[6], (HEADS,), jnp.float32) ** levels(seeds[6], (HEADS,), ((0, 2),), -0.2, 0.2), 0.3, 0.8)
    head_gain = jnp.clip(1.0 + 0.18 * jax.random.normal(seeds[7], (VD,), jnp.float32), 0.1, 1.9)
    out_weight = normal_values(seeds[8], (HEADS * VD, D), (HEADS * VD) ** -0.5, 0.1875)
    norm_gain = jnp.clip(1.0 + 0.18 * jax.random.normal(seeds[9], (D,), jnp.float32), 0.1, 1.9)
    route_ids_keys = jax.random.split(jax.random.fold_in(seeds[10], 1), TOKENS // (TOK_DEV // N_TP))
    route_ids_turns = jax.random.permutation(jax.random.fold_in(seeds[10], 3), TOKENS // (TOK_DEV // N_TP))
    route_ids = jax.vmap(lambda own, number: routed_block(jax.random.fold_in(seeds[10], 2), own, number, TOK_DEV // N_TP, EXPERTS, TOPK, CAP, 2))(route_ids_keys, route_ids_turns).reshape((TOKENS, TOPK))
    route_weights = jnp.clip(0.25 + 0.75 * jax.random.uniform(seeds[11], (TOKENS, TOPK), jnp.float32) ** levels(seeds[11], (TOKENS, TOPK), ((0, 32),), -0.2, 0.2), 0.25, 1.0)
    gate_weight = normal_values(seeds[12], (EXPERTS, D, FF), D ** -0.5, 0.125, ((0, 16), (2, 2)))
    up_weight = normal_values(seeds[13], (EXPERTS, D, FF), D ** -0.5, 0.125, ((0, 16), (2, 2)))
    down_weight = normal_values(seeds[14], (EXPERTS, FF, D), FF ** -0.5, 0.25, ((0, 16), (1, 2)))
    return dict(residual=residual, query_one=query_one, key_one=key_one, query_two=query_two, key_two=key_two, value_rows=value_rows, lambda_head=lambda_head, head_gain=head_gain, out_weight=out_weight, norm_gain=norm_gain, route_ids=route_ids, route_weights=route_weights, gate_weight=gate_weight, up_weight=up_weight, down_weight=down_weight)


epsilon = 1e-06

def settle(values):
    return lax.optimization_barrier(values.astype(jnp.bfloat16)).astype(jnp.float32)

def head_map(inputs, allowed):
    queries, keys, value_part = inputs
    scores = jnp.dot(queries, keys.T) * HD ** (-0.5)
    scores = jnp.where(allowed, scores, -jnp.inf)
    highest = lax.optimization_barrier(jnp.max(scores, axis=-1, keepdims=True))
    exp_weights = jnp.where(allowed, jnp.exp(scores - highest), 0.0)
    row_total = lax.optimization_barrier(jnp.sum(exp_weights, axis=-1, keepdims=True))
    summed = jnp.dot(settle(exp_weights), value_part)
    return summed / row_total

def one_map(queries, keys, value_part, allowed):
    head_queries = jnp.transpose(queries, (1, 0, 2))
    head_keys = jnp.transpose(keys, (1, 0, 2))
    head_values = jnp.transpose(value_part, (1, 0, 2))
    result = lax.map(lambda inputs: head_map(inputs, allowed), (head_queries, head_keys, head_values))
    return jnp.transpose(result, (1, 0, 2))

def attention(query_one, key_one, query_two, key_two, value_rows, lambda_head, head_gain):
    first_query = query_one.astype(jnp.float32).reshape(TOKENS, HEADS, HD)
    first_key = key_one.astype(jnp.float32).reshape(TOKENS, HEADS, HD)
    second_query = query_two.astype(jnp.float32).reshape(TOKENS, HEADS, HD)
    second_key = key_two.astype(jnp.float32).reshape(TOKENS, HEADS, HD)
    value_part = value_rows.astype(jnp.float32).reshape(TOKENS, HEADS, VD)
    outputs = []
    for segment in range(N_SP):
        begin_row = segment * TOK_DEV
        end_row = begin_row + TOK_DEV
        allowed = (begin_row + jnp.arange(TOK_DEV))[:, None] >= jnp.arange(end_row)[None, :]
        first_out = one_map(first_query[begin_row:end_row], first_key[:end_row], value_part[:end_row], allowed)
        second_out = one_map(second_query[begin_row:end_row], second_key[:end_row], value_part[:end_row], allowed)
        head_out = first_out - lambda_head[None, :, None] * second_out
        normed = head_out * lax.rsqrt(lax.optimization_barrier(jnp.mean(head_out * head_out, axis=-1, keepdims=True)) + epsilon) * head_gain
        outputs.append(normed.reshape(TOK_DEV, HEADS * VD).astype(jnp.bfloat16))
    return jnp.concatenate(outputs, axis=0)

def experts(routed, route_ids, route_weights, gate_weight, up_weight, down_weight):
    flat_ids = route_ids.reshape(-1).astype(jnp.int32)
    flat_weights = route_weights.reshape(-1)
    most_rows = N_SP * N_TP * CAP
    group_width = FF // N_TP

    def expert_step(totals, inputs):
        index, gate_one, up_one, down_one = inputs
        hits = flat_ids == index
        picked = jnp.nonzero(hits, size=most_rows, fill_value=0)[0].astype(jnp.int32)
        valid = jnp.arange(most_rows) < jnp.sum(hits.astype(jnp.int32))
        token_rows = picked // TOPK
        input_rows = routed[token_rows]
        gate = jnp.dot(input_rows, gate_one, preferred_element_type=jnp.float32)
        upper = jnp.dot(input_rows, up_one, preferred_element_type=jnp.float32)
        hidden = (jax.nn.silu(gate) * upper).astype(jnp.bfloat16)
        summed = jnp.zeros((most_rows, D), jnp.float32)
        for group in range(N_TP):
            begin_col = group * group_width
            partial_value = jnp.dot(hidden[:, begin_col:begin_col + group_width], down_one[begin_col:begin_col + group_width], preferred_element_type=jnp.float32)
            summed = summed + settle(partial_value)
        result = settle(summed)
        weight = jnp.where(valid, flat_weights[picked], 0.0)
        totals = totals.at[token_rows].add(weight[:, None] * result)
        return (totals, None)
    steps_in = (jnp.arange(EXPERTS, dtype=jnp.int32), gate_weight, up_weight, down_weight)
    return lax.scan(expert_step, jnp.zeros((TOKENS, D), jnp.float32), steps_in)[0]

def reference(residual, query_one, key_one, query_two, key_two, value_rows, lambda_head, head_gain, out_weight, norm_gain, route_ids, route_weights, gate_weight, up_weight, down_weight):
    attended = attention(query_one, key_one, query_two, key_two, value_rows, lambda_head, head_gain)
    after = (residual.astype(jnp.float32) + jnp.dot(attended, out_weight, preferred_element_type=jnp.float32)).astype(jnp.bfloat16)
    after_float = after.astype(jnp.float32)
    routed = (after_float * lax.rsqrt(lax.optimization_barrier(jnp.mean(after_float * after_float, axis=-1, keepdims=True)) + epsilon) * norm_gain).astype(jnp.bfloat16)
    moe_out = experts(routed, route_ids, route_weights, gate_weight, up_weight, down_weight)
    return (after_float + moe_out).astype(jnp.bfloat16)
```

```python
import functools

import jax
import jax.numpy as jnp
from jax import lax
from jax.experimental import pallas as pl
from jax.experimental.pallas import tpu as pltpu
from jax.sharding import PartitionSpec as P

MESH = pl.DeviceIdType.MESH
EPS = 1e-06
LOW = -1e30
BF = jnp.bfloat16
F32 = jnp.float32
ANY = pl.BlockSpec(memory_space=pl.ANY)
VM = pl.BlockSpec(memory_space=pltpu.VMEM)
DMA = pltpu.SemaphoreType.DMA


def rcopy(src, dst, ssem, rsem, peer):
    return pltpu.make_async_remote_copy(
        src_ref=src, dst_ref=dst, send_sem=ssem, recv_sem=rsem, device_id=peer, device_id_type=MESH
    )


def greet(peers):
    barrier = pltpu.get_barrier_semaphore()
    for peer in peers:
        pl.semaphore_signal(barrier, inc=1, device_id=peer, device_id_type=MESH)
    pl.semaphore_wait(barrier, len(peers))


def pack_kernel(nh, q1, k1, q2, k2, v, q_out, kv_out):
    hd = q1.shape[1] // nh
    vd = v.shape[1] // nh
    scale = hd ** (-0.5)
    for h in range(nh):
        a, b = h * hd, (h + 1) * hd
        q = jnp.concatenate([q1[:, a:b], q2[:, a:b]], axis=1).astype(F32) * scale
        q_out[h] = q.astype(BF)
        kv_out[h, :, : 2 * hd] = jnp.concatenate([k1[:, a:b], k2[:, a:b]], axis=1)
        kv_out[h, :, 2 * hd :] = v[:, h * vd : (h + 1) * vd]


def gather_kernel(
    n, nh, q_ref, kv_ref, g_ref, u_ref, d_ref, q_out, kv_out, g_out, u_out, d_out,
    qs, qr, ks, kr, fs, fr, ws, wr, ls,
):
    np_ = n // nh
    m = np_.bit_length() - 1
    s = lax.axis_index("sp")
    t = lax.axis_index("tp")
    zi = s // np_
    r = s % np_

    def flip(x, bit):
        w = 1 << bit
        return x + w * (1 - 2 * ((x // w) % 2))

    zpeers = [None] + [((zi + d) % nh) for d in range(1, nh)]
    peers = [(zp * np_ + r, t) for zp in zpeers[1:]]
    peers += [(zi * np_ + flip(r, b), t) for b in range(m)]
    peers += [(s, 1 - t)]
    greet(peers)

    own_kv = pltpu.make_async_copy(kv_ref.at[zi], kv_out.at[s], ls.at[0])
    own_q = pltpu.make_async_copy(q_ref.at[zi], q_out.at[zi], ls.at[1])
    own_kv.start()
    own_q.start()
    kcopies, qcopies = [None], []
    for d in range(1, nh):
        zp = zpeers[d]
        c = rcopy(kv_ref.at[zp], kv_out.at[s], ks.at[d], kr.at[d], (zp * np_ + r, t))
        c.start()
        kcopies.append(c)
    for d in range(1, nh):
        zp = zpeers[d]
        c = rcopy(q_ref.at[zp], q_out.at[zi], qs.at[d], qr.at[d], (zp * np_ + r, t))
        c.start()
        qcopies.append(c)
    wcopies = []
    for i, (a, b) in enumerate(((g_ref, g_out), (u_ref, u_out), (d_ref, d_out))):
        c = rcopy(a, b, ws.at[i], wr.at[i], (s, 1 - t))
        c.start()
        wcopies.append(c)
    own_kv.wait()

    def phase(d, p):
        base = ((zi + nh - d) % nh) * np_
        peer = (zi * np_ + flip(r, (p + d) % m), t)
        out = []
        for c in range(1 << p):
            rr = r
            for b in range(p):
                if (c >> b) & 1:
                    rr = flip(rr, (b + d) % m)
            i = d * (np_ - 1) + (1 << p) - 1 + c
            blk = kv_out.at[base + rr]
            e = rcopy(blk, blk, fs.at[i], fr.at[i], peer)
            out.append(e)
        return out

    live = {}
    for d in range(nh):
        if d:
            kcopies[d].wait_recv()
        live[d, 0] = phase(d, 0)
        for e in live[d, 0]:
            e.start()
    for p in range(1, m):
        for d in range(nh):
            for e in live[d, p - 1]:
                e.wait_recv()
            live[d, p] = phase(d, p)
            for e in live[d, p]:
                e.start()
    for d in range(nh):
        for e in live[d, m - 1]:
            e.wait_recv()
        for p in range(m):
            for e in live[d, p]:
                e.wait_send()
    for c in kcopies[1:]:
        c.wait_send()
    for c in qcopies + wcopies:
        c.wait()
    own_q.wait()


def attention_kernel(np_, q_ref, kv_ref, lam_ref, gain_ref, out_ref):
    s = lax.axis_index("sp")
    jq = pl.program_id(0) * np_ + s % np_
    zi = s // np_
    rows, two = q_ref.shape[1], q_ref.shape[2]
    hd = two // 2
    vd = kv_ref.shape[2] - two
    q = q_ref[0]
    lane = lax.broadcasted_iota(jnp.int32, (rows, two), 1)
    zero = jnp.zeros((), BF)
    qs = (jnp.where(lane < hd, q, zero), jnp.where(lane >= hd, q, zero))

    def step(j, state, masked):
        k = kv_ref[j, :, :two]
        v = kv_ref[j, :, two:]
        out = []
        for i in range(2):
            mx, l, acc = state[i]
            sc = lax.dot_general(qs[i], k, (((1,), (1,)), ((), ())), preferred_element_type=F32)
            if masked:
                ri = lax.broadcasted_iota(jnp.int32, sc.shape, 0)
                ci = lax.broadcasted_iota(jnp.int32, sc.shape, 1)
                sc = jnp.where(ri >= ci, sc, LOW)
            new = jnp.maximum(mx, jnp.max(sc, axis=1, keepdims=True))
            p = jnp.exp(sc - new)
            f = jnp.exp(mx - new)
            l = l * f + jnp.sum(p, axis=1, keepdims=True)
            acc = acc * f + jnp.dot(p.astype(BF), v, preferred_element_type=F32)
            out.append((new, l, acc))
        return tuple(out)

    empty = (jnp.full((rows, 1), LOW, F32), jnp.zeros((rows, 1), F32), jnp.zeros((rows, vd), F32))
    state = lax.fori_loop(0, jq, lambda j, st: step(j, st, False), (empty, empty))
    (_, l1, a1), (_, l2, a2) = step(jq, state, True)
    o = a1 / l1 - lam_ref[zi] * (a2 / l2)
    o = o * lax.rsqrt(jnp.mean(o * o, axis=1, keepdims=True) + EPS) * gain_ref[...]
    out_ref[0] = o.astype(BF)


def heads_kernel(n, nt, nh, o_ref, a_ref, ss, rs, ls):
    np_ = n // nh
    s = lax.axis_index("sp")
    t = lax.axis_index("tp")
    zi = s // np_
    r = s % np_
    half = o_ref.shape[1] // nt
    vd = o_ref.shape[2]
    cols = pl.ds(pl.multiple_of((t * nh + zi) * vd, vd), vd)
    combos = [(dz, dt) for dz in range(nh) for dt in range(nt) if dz or dt]
    where = [((zi + dz) % nh, (t + dt) % nt) for dz, dt in combos]
    greet([(z * np_ + r, tp) for z, tp in where])
    own = pltpu.make_async_copy(
        o_ref.at[zi, pl.ds(pl.multiple_of(t * half, half), half)], a_ref.at[:, cols], ls
    )
    own.start()
    copies = []
    for i, (z, tp) in enumerate(where):
        c = rcopy(
            o_ref.at[z, pl.ds(pl.multiple_of(tp * half, half), half)],
            a_ref.at[:, cols], ss.at[i], rs.at[i], (z * np_ + r, tp),
        )
        c.start()
        copies.append(c)
    own.wait()
    for c in copies:
        c.wait()


def route_kernel(ne, cap, capp, a_ref, w_ref, res_ref, gain_ref, ids_ref, after_ref, d0_ref, d1_ref, out_ref):
    rows = a_ref.shape[0]
    proj = jnp.dot(a_ref[...], w_ref[...], preferred_element_type=F32)
    after = (res_ref[...].astype(F32) + proj).astype(BF)
    after_ref[...] = after
    af = after.astype(F32)
    routed = (
        af * lax.rsqrt(jnp.mean(af * af, axis=1, keepdims=True) + EPS) * gain_ref[...]
    ).astype(BF)
    slots = ne * capp
    ids = ids_ref[...]
    ex = lax.broadcasted_iota(jnp.int32, (rows, ne), 1)
    oh0 = (ids[:, 0:1] == ex).astype(F32)
    oh1 = (ids[:, 1:2] == ex).astype(F32)
    tri = (
        lax.broadcasted_iota(jnp.int32, (rows, rows), 0)
        > lax.broadcasted_iota(jnp.int32, (rows, rows), 1)
    ).astype(F32).astype(BF)
    rank = jnp.dot(tri, (oh0 + oh1).astype(BF), preferred_element_type=F32)
    er = lax.broadcasted_iota(jnp.int32, (ne, slots), 0) * capp
    sl = lax.broadcasted_iota(jnp.int32, (ne, slots), 1)
    place = sl - er
    spread = ((place >= 0) & (place < capp)).astype(F32)
    sb = spread.astype(BF)
    slot_in = jnp.sum(jnp.where(spread > 0.0, place.astype(F32), 0.0), axis=0, keepdims=True)
    rank_x = jnp.dot(rank.astype(BF), sb, preferred_element_type=F32)
    hit = jnp.where(rank_x == slot_in, 1.0, 0.0)
    d0 = (jnp.dot(oh0.astype(BF), sb, preferred_element_type=F32) * hit).astype(BF)
    d1 = (jnp.dot(oh1.astype(BF), sb, preferred_element_type=F32) * hit).astype(BF)
    d0_ref[...] = d0
    d1_ref[...] = d1
    out_ref[...] = lax.dot_general(
        d0 + d1, routed, (((0,), (0,)), ((), ())), preferred_element_type=F32
    ).astype(BF)


def swap_kernel(n, x_ref, y_ref, stage, ss, rs, ls):
    s = lax.axis_index("sp")
    t = lax.axis_index("tp")
    greet([((s + d) % n, t) for d in range(1, n)])
    copies = []
    for d in range(1, n):
        p = (s + d) % n
        c = rcopy(x_ref.at[p], y_ref.at[s], ss.at[d], rs.at[d], (p, t))
        c.start()
        copies.append(c)
    a = pltpu.make_async_copy(x_ref.at[s], stage, ls.at[0])
    a.start()
    a.wait()
    b = pltpu.make_async_copy(stage, y_ref.at[s], ls.at[1])
    b.start()
    b.wait()
    for c in copies:
        c.wait()


def swap(x, n, cid):
    return pl.pallas_call(
        functools.partial(swap_kernel, n),
        out_shape=jax.ShapeDtypeStruct(x.shape, x.dtype),
        in_specs=[ANY],
        out_specs=ANY,
        scratch_shapes=[pltpu.VMEM(x.shape[1:], x.dtype), DMA((n,)), DMA((n,)), DMA((2,))],
        compiler_params=pltpu.CompilerParams(collective_id=cid, has_side_effects=True),
        name="swap%d" % cid,
    )(x)


def ffn_kernel(x_ref, g1, u1, d1, g2, u2, d2, y_ref):
    x = x_ref[...]
    total = None
    for g, u, d in ((g1, u1, d1), (g2, u2, d2)):
        gate = jnp.dot(x, g[...], preferred_element_type=F32)
        up = jnp.dot(x, u[...], preferred_element_type=F32)
        hid = (gate * jax.nn.sigmoid(gate) * up).astype(BF)
        part = jnp.dot(hid, d[...], preferred_element_type=F32)
        total = part if total is None else total + part
    y_ref[...] = total.astype(BF)


def combine_kernel(ret_ref, d0_ref, d1_ref, rw_ref, after_ref, out_ref):
    ret = ret_ref[...]
    rw = rw_ref[...]
    a = jnp.dot(d0_ref[...], ret, preferred_element_type=F32) * rw[:, 0:1]
    b = jnp.dot(d1_ref[...], ret, preferred_element_type=F32) * rw[:, 1:2]
    out_ref[...] = (after_ref[...].astype(F32) + (a + b)).astype(BF)


def on_device(
    residual, query_one, key_one, query_two, key_two, value_rows, lambda_head, head_gain,
    out_weight, norm_gain, route_ids, route_weights, gate_weight, up_weight, down_weight,
):
    n = lax.axis_size("sp")
    nt = lax.axis_size("tp")
    nh = lambda_head.shape[0]
    np_ = n // nh
    rows = query_one.shape[0]
    hd = query_one.shape[1] // nh
    vd = value_rows.shape[1] // nh
    wid = residual.shape[1]
    local = residual.shape[0]
    sds = jax.ShapeDtypeStruct

    q, kv = pl.pallas_call(
        functools.partial(pack_kernel, nh),
        out_shape=(sds((nh, rows, 2 * hd), BF), sds((nh, rows, 2 * hd + vd), BF)),
        in_specs=[VM] * 5,
        out_specs=(VM, VM),
        name="pack",
    )(query_one, key_one, query_two, key_two, value_rows)

    g, u, dn = gate_weight[0], up_weight[0], down_weight[0]
    nf = nh * (np_ - 1)
    q_all, kv_all, g2, u2, dn2 = pl.pallas_call(
        functools.partial(gather_kernel, n, nh),
        out_shape=(
            sds((nh, rows, 2 * hd), BF), sds((n, rows, 2 * hd + vd), BF),
            sds(g.shape, BF), sds(u.shape, BF), sds(dn.shape, BF),
        ),
        in_specs=[VM, VM, ANY, ANY, ANY],
        out_specs=(VM, VM, ANY, ANY, ANY),
        scratch_shapes=[
            DMA((nh,)), DMA((nh,)), DMA((nh,)), DMA((nh,)), DMA((nf,)), DMA((nf,)),
            DMA((3,)), DMA((3,)), DMA((2,)),
        ],
        compiler_params=pltpu.CompilerParams(collective_id=1, has_side_effects=True),
        name="gather_heads",
    )(q, kv, g, u, dn)

    attended = pl.pallas_call(
        functools.partial(attention_kernel, np_),
        out_shape=sds((nh, rows, vd), BF),
        grid=(nh,),
        in_specs=[
            pl.BlockSpec((1, rows, 2 * hd), lambda i: (i, 0, 0)),
            VM,
            pl.BlockSpec(memory_space=pltpu.SMEM),
            VM,
        ],
        out_specs=pl.BlockSpec((1, rows, vd), lambda i: (i, 0, 0)),
        name="attend",
    )(q_all, kv_all, lambda_head, head_gain.reshape(1, vd))

    na = nh * nt - 1
    all_heads = pl.pallas_call(
        functools.partial(heads_kernel, n, nt, nh),
        out_shape=sds((rows // nt, nh * nt * vd), BF),
        in_specs=[VM],
        out_specs=VM,
        scratch_shapes=[DMA((na,)), DMA((na,)), DMA],
        compiler_params=pltpu.CompilerParams(collective_id=2, has_side_effects=True),
        name="return_heads",
    )(attended)

    ne = gate_weight.shape[0] * n
    cap = max(2, (3 * rows + 2 * n - 1) // (2 * n))
    capp = (cap + 7) // 8 * 8
    slots = ne * capp
    after, d0, d1, outgoing = pl.pallas_call(
        functools.partial(route_kernel, ne, cap, capp),
        out_shape=(
            sds((local, wid), BF), sds((local, slots), BF), sds((local, slots), BF), sds((slots, wid), BF),
        ),
        in_specs=[VM] * 5,
        out_specs=(VM, VM, VM, VM),
        name="project_route",
    )(all_heads, out_weight, residual, norm_gain.reshape(1, wid), route_ids)

    arrived = swap(outgoing.reshape(ne, capp, wid), n, 3)

    tile = slots // 2
    full = lambda i: (0, 0)
    y = pl.pallas_call(
        ffn_kernel,
        out_shape=sds((slots, wid), BF),
        grid=(2,),
        in_specs=[pl.BlockSpec((tile, wid), lambda i: (i, 0))] + [VM] * 6,
        out_specs=pl.BlockSpec((tile, wid), lambda i: (i, 0)),
        name="ffn",
    )(arrived.reshape(slots, wid), g, u, dn, g2, u2, dn2)

    returned = swap(y.reshape(ne, capp, wid), n, 4)

    return pl.pallas_call(
        combine_kernel,
        out_shape=sds((local, wid), BF),
        in_specs=[VM] * 5,
        out_specs=VM,
        name="combine",
    )(returned.reshape(slots, wid), d0, d1, route_weights, after)


def solution(mesh):
    placed = (
        P(("sp", "tp"), None), P("sp", "tp"), P("sp", "tp"), P("sp", "tp"), P("sp", "tp"),
        P("sp", "tp"), P("tp"), P(), P(), P(), P(("sp", "tp"), None), P(("sp", "tp"), None),
        P("sp", None, "tp"), P("sp", None, "tp"), P("sp", "tp", None),
    )
    return jax.shard_map(
        on_device, mesh=mesh, in_specs=placed, out_specs=P(("sp", "tp"), None), check_vma=False
    )
```

```python
import functools

import jax
import jax.numpy as jnp
from jax import lax
from jax.experimental import pallas as pl
from jax.experimental.pallas import tpu as pltpu
from jax.sharding import PartitionSpec as P

MESH = pl.DeviceIdType.MESH
EPS = 1e-06
LOW = -1e30
BF = jnp.bfloat16
F32 = jnp.float32
ANY = pl.BlockSpec(memory_space=pl.ANY)
VM = pl.BlockSpec(memory_space=pltpu.VMEM)
DMA = pltpu.SemaphoreType.DMA


def rcopy(src, dst, ssem, rsem, peer):
    return pltpu.make_async_remote_copy(
        src_ref=src, dst_ref=dst, send_sem=ssem, recv_sem=rsem, device_id=peer, device_id_type=MESH
    )


def greet(peers):
    barrier = pltpu.get_barrier_semaphore()
    for peer in peers:
        pl.semaphore_signal(barrier, inc=1, device_id=peer, device_id_type=MESH)
    pl.semaphore_wait(barrier, len(peers))


def pack_kernel(nh, q1, k1, q2, k2, v, q_out, kv_out):
    hd = q1.shape[1] // nh
    vd = v.shape[1] // nh
    scale = hd ** (-0.5)
    for h in range(nh):
        a, b = h * hd, (h + 1) * hd
        q = jnp.concatenate([q1[:, a:b], q2[:, a:b]], axis=1).astype(F32) * scale
        q_out[h] = q.astype(BF)
        kv_out[h, :, : 2 * hd] = jnp.concatenate([k1[:, a:b], k2[:, a:b]], axis=1)
        kv_out[h, :, 2 * hd :] = v[:, h * vd : (h + 1) * vd]


def gather_kernel(
    n, nh, q_ref, kv_ref, g_ref, u_ref, d_ref, q_out, kv_out, g_out, u_out, d_out,
    qs, qr, ks, kr, fs, fr, ws, wr, ls,
):
    np_ = n // nh
    m = np_.bit_length() - 1
    s = lax.axis_index("sp")
    t = lax.axis_index("tp")
    zi = s // np_
    r = s % np_

    def flip(x, bit):
        w = 1 << bit
        return x + w * (1 - 2 * ((x // w) % 2))

    zpeers = [None] + [((zi + d) % nh) for d in range(1, nh)]
    peers = [(zp * np_ + r, t) for zp in zpeers[1:]]
    peers += [(zi * np_ + flip(r, b), t) for b in range(m)]
    peers += [(s, 1 - t)]
    greet(peers)

    own_kv = pltpu.make_async_copy(kv_ref.at[zi], kv_out.at[s], ls.at[0])
    own_q = pltpu.make_async_copy(q_ref.at[zi], q_out.at[zi], ls.at[1])
    own_kv.start()
    own_q.start()
    kcopies, qcopies = [None], []
    for d in range(1, nh):
        zp = zpeers[d]
        c = rcopy(kv_ref.at[zp], kv_out.at[s], ks.at[d], kr.at[d], (zp * np_ + r, t))
        c.start()
        kcopies.append(c)
    for d in range(1, nh):
        zp = zpeers[d]
        c = rcopy(q_ref.at[zp], q_out.at[zi], qs.at[d], qr.at[d], (zp * np_ + r, t))
        c.start()
        qcopies.append(c)
    wcopies = []
    for i, (a, b) in enumerate(((g_ref, g_out), (u_ref, u_out), (d_ref, d_out))):
        c = rcopy(a, b, ws.at[i], wr.at[i], (s, 1 - t))
        c.start()
        wcopies.append(c)
    own_kv.wait()

    def phase(d, p):
        base = ((zi + nh - d) % nh) * np_
        peer = (zi * np_ + flip(r, (p + d) % m), t)
        out = []
        for c in range(1 << p):
            rr = r
            for b in range(p):
                if (c >> b) & 1:
                    rr = flip(rr, (b + d) % m)
            i = d * (np_ - 1) + (1 << p) - 1 + c
            blk = kv_out.at[base + rr]
            e = rcopy(blk, blk, fs.at[i], fr.at[i], peer)
            out.append(e)
        return out

    live = {}
    for d in range(nh):
        if d:
            kcopies[d].wait_recv()
        live[d, 0] = phase(d, 0)
        for e in live[d, 0]:
            e.start()
    for p in range(1, m):
        for d in range(nh):
            for e in live[d, p - 1]:
                e.wait_recv()
            live[d, p] = phase(d, p)
            for e in live[d, p]:
                e.start()
    for d in range(nh):
        for e in live[d, m - 1]:
            e.wait_recv()
        for p in range(m):
            for e in live[d, p]:
                e.wait_send()
    for c in kcopies[1:]:
        c.wait_send()
    for c in qcopies + wcopies:
        c.wait()
    own_q.wait()


def attention_kernel(np_, q_ref, kv_ref, lam_ref, gain_ref, out_ref, s_scr, m_scr, acc_scr):
    s = lax.axis_index("sp")
    jq = pl.program_id(0) * np_ + s % np_
    zi = s // np_
    rows, two = q_ref.shape[1], q_ref.shape[2]
    hd = two // 2
    vd = kv_ref.shape[2] - two
    group = min(np_, 4)
    q = q_ref[0]
    lane = lax.broadcasted_iota(jnp.int32, (rows, two), 1)
    zero = jnp.zeros((), BF)
    qs = jnp.concatenate([jnp.where(lane < hd, q, zero), jnp.where(lane >= hd, q, zero)], axis=0)
    m_scr[...] = jnp.full(m_scr.shape, LOW, F32)
    acc_scr[...] = jnp.zeros(acc_scr.shape, F32)
    lanes = m_scr.shape[1]

    def score(j0, count, masked):
        best = m_scr[...]
        for c in range(count):
            k = kv_ref[j0 + c, :, :two]
            sc = lax.dot_general(qs, k, (((1,), (1,)), ((), ())), preferred_element_type=F32)
            if masked:
                ri = lax.broadcasted_iota(jnp.int32, (rows, rows), 0)
                ci = lax.broadcasted_iota(jnp.int32, (rows, rows), 1)
                ok = ri >= ci
                sc = jnp.concatenate(
                    [jnp.where(ok, sc[:rows], LOW), jnp.where(ok, sc[rows:], LOW)], axis=0
                )
            s_scr[j0 + c] = sc
            for i in range(rows // lanes):
                best = jnp.maximum(best, sc[:, i * lanes : (i + 1) * lanes])
        m_scr[...] = best

    def weigh(j0, count):
        top = m_scr[...]
        parts = []
        for c in range(count):
            sc = s_scr[j0 + c]
            for i in range(rows // lanes):
                parts.append(jnp.exp(sc[:, i * lanes : (i + 1) * lanes] - top).astype(BF))
        p = jnp.concatenate(parts, axis=1)
        v = kv_ref[pl.ds(j0, count), :, two:].reshape(count * rows, vd)
        v = jnp.concatenate([v, jnp.ones((count * rows, vd), BF)], axis=1)
        acc_scr[...] += jnp.dot(p, v, preferred_element_type=F32)

    def loop(lo, hi, fn):
        lax.fori_loop(lo, hi, lambda j, c: (fn(j), c)[1], 0)

    groups = jq // group
    loop(0, groups, lambda j: score(j * group, group, False))
    loop(groups * group, jq, lambda j: score(j, 1, False))
    score(jq, 1, True)
    m_scr[...] = jnp.broadcast_to(jnp.max(m_scr[...], axis=1, keepdims=True), m_scr.shape)
    loop(0, groups, lambda j: weigh(j * group, group))
    loop(groups * group, jq + 1, lambda j: weigh(j, 1))
    a1 = acc_scr[:rows, :vd] / acc_scr[:rows, vd:]
    a2 = acc_scr[rows:, :vd] / acc_scr[rows:, vd:]
    o = a1 - lam_ref[zi] * a2
    o = o * lax.rsqrt(jnp.mean(o * o, axis=1, keepdims=True) + EPS) * gain_ref[...]
    out_ref[0] = o.astype(BF)


def heads_kernel(n, nt, nh, o_ref, a_ref, ss, rs, ls):
    np_ = n // nh
    s = lax.axis_index("sp")
    t = lax.axis_index("tp")
    zi = s // np_
    r = s % np_
    half = o_ref.shape[1] // nt
    vd = o_ref.shape[2]
    cols = pl.ds(pl.multiple_of((t * nh + zi) * vd, vd), vd)
    combos = [(dz, dt) for dz in range(nh) for dt in range(nt) if dz or dt]
    where = [((zi + dz) % nh, (t + dt) % nt) for dz, dt in combos]
    greet([(z * np_ + r, tp) for z, tp in where])
    own = pltpu.make_async_copy(
        o_ref.at[zi, pl.ds(pl.multiple_of(t * half, half), half)], a_ref.at[:, cols], ls
    )
    own.start()
    copies = []
    for i, (z, tp) in enumerate(where):
        c = rcopy(
            o_ref.at[z, pl.ds(pl.multiple_of(tp * half, half), half)],
            a_ref.at[:, cols], ss.at[i], rs.at[i], (z * np_ + r, tp),
        )
        c.start()
        copies.append(c)
    own.wait()
    for c in copies:
        c.wait()


def route_kernel(ne, cap, capp, a_ref, w_ref, res_ref, gain_ref, ids_ref, after_ref, d0_ref, d1_ref, out_ref):
    rows = a_ref.shape[0]
    proj = jnp.dot(a_ref[...], w_ref[...], preferred_element_type=F32)
    after = (res_ref[...].astype(F32) + proj).astype(BF)
    after_ref[...] = after
    af = after.astype(F32)
    routed = (
        af * lax.rsqrt(jnp.mean(af * af, axis=1, keepdims=True) + EPS) * gain_ref[...]
    ).astype(BF)
    slots = ne * capp
    ids = ids_ref[...]
    ex = lax.broadcasted_iota(jnp.int32, (rows, ne), 1)
    oh0 = (ids[:, 0:1] == ex).astype(F32)
    oh1 = (ids[:, 1:2] == ex).astype(F32)
    tri = (
        lax.broadcasted_iota(jnp.int32, (rows, rows), 0)
        > lax.broadcasted_iota(jnp.int32, (rows, rows), 1)
    ).astype(F32).astype(BF)
    rank = jnp.dot(tri, (oh0 + oh1).astype(BF), preferred_element_type=F32)
    er = lax.broadcasted_iota(jnp.int32, (ne, slots), 0) * capp
    sl = lax.broadcasted_iota(jnp.int32, (ne, slots), 1)
    place = sl - er
    spread = ((place >= 0) & (place < capp)).astype(F32)
    sb = spread.astype(BF)
    slot_in = jnp.sum(jnp.where(spread > 0.0, place.astype(F32), 0.0), axis=0, keepdims=True)
    rank_x = jnp.dot(rank.astype(BF), sb, preferred_element_type=F32)
    hit = jnp.where(rank_x == slot_in, 1.0, 0.0)
    d0 = (jnp.dot(oh0.astype(BF), sb, preferred_element_type=F32) * hit).astype(BF)
    d1 = (jnp.dot(oh1.astype(BF), sb, preferred_element_type=F32) * hit).astype(BF)
    d0_ref[...] = d0
    d1_ref[...] = d1
    out_ref[...] = lax.dot_general(
        d0 + d1, routed, (((0,), (0,)), ((), ())), preferred_element_type=F32
    ).astype(BF)


def moe_kernel(
    n, nz, x_ref, g1, u1, d1, g2, u2, d2, d0_ref, d1_ref, rw_ref, after_ref, out_ref,
    arr, ys, ret, gw, uw, dw, ss, rs, bs, br, ls, ws,
):
    np_ = n // nz
    s = lax.axis_index("sp")
    t = lax.axis_index("tp")
    zi = s // np_
    r = s % np_
    capp, wid = arr.shape[1], arr.shape[2]

    def plane(mask):
        z = zi
        for b in range(nz.bit_length() - 1):
            if (mask >> b) & 1:
                w = 1 << b
                z = z + w * (1 - 2 * ((zi // w) % 2))
        return z

    greet([((s + d) % n, t) for d in range(1, n)])
    masks = list(range(nz - 1, -1, -1))
    sends, backs, selfs = {}, {}, []
    for w in masks:
        sends[w] = []
        for c in range(np_):
            if w == 0 and c == 0:
                e = pltpu.make_async_copy(x_ref.at[s], arr.at[s], ls.at[0])
                e.start()
                selfs.append(e)
                continue
            p = plane(w) * np_ + (r + c) % np_
            i = w * np_ + c
            e = rcopy(x_ref.at[p], arr.at[s], ss.at[i], rs.at[i], (p, t))
            e.start()
            sends[w].append(e)
    loads = []
    for i, (a, b) in enumerate(
        ((g1, gw.at[0]), (g2, gw.at[1]), (u1, uw.at[0]), (u2, uw.at[1]), (d1, dw.at[0]), (d2, dw.at[1]))
    ):
        e = pltpu.make_async_copy(a, b, ws.at[i])
        e.start()
        loads.append(e)
    for e in loads:
        e.wait()

    order = [nz - 1, 0] + list(range(1, nz - 1))
    for w in order:
        for e in sends[w]:
            e.wait_recv()
        if w == 0:
            selfs[0].wait()
        base = plane(w) * np_
        x = arr[pl.ds(base, np_)].astype(F32).reshape(np_ * capp, wid).astype(BF)
        total = None
        for i in range(2):
            gate = jnp.dot(x, gw[i], preferred_element_type=F32)
            up = jnp.dot(x, uw[i], preferred_element_type=F32)
            hid = (gate * jax.nn.sigmoid(gate) * up).astype(BF)
            part = jnp.dot(hid, dw[i], preferred_element_type=F32)
            total = part if total is None else total + part
        ys[pl.ds(base, np_)] = total.reshape(np_, capp, wid).astype(BF)
        backs[w] = []
        for c in range(np_):
            if w == 0 and c == 0:
                e = pltpu.make_async_copy(ys.at[s], ret.at[s], ls.at[1])
                e.start()
                selfs.append(e)
                continue
            p = base + (r + c) % np_
            i = w * np_ + c
            e = rcopy(ys.at[p], ret.at[s], bs.at[i], br.at[i], (p, t))
            e.start()
            backs[w].append(e)
    for w in order:
        for e in backs[w]:
            e.wait_recv()
    selfs[1].wait()
    back = ret[...].astype(F32).reshape(n * capp, wid).astype(BF)
    rw = rw_ref[...]
    a = jnp.dot(d0_ref[...], back, preferred_element_type=F32) * rw[:, 0:1]
    b = jnp.dot(d1_ref[...], back, preferred_element_type=F32) * rw[:, 1:2]
    out_ref[...] = (after_ref[...].astype(F32) + (a + b)).astype(BF)
    for w in order:
        for e in sends[w] + backs[w]:
            e.wait_send()


def on_device(
    residual, query_one, key_one, query_two, key_two, value_rows, lambda_head, head_gain,
    out_weight, norm_gain, route_ids, route_weights, gate_weight, up_weight, down_weight,
):
    n = lax.axis_size("sp")
    nt = lax.axis_size("tp")
    nh = lambda_head.shape[0]
    np_ = n // nh
    rows = query_one.shape[0]
    hd = query_one.shape[1] // nh
    vd = value_rows.shape[1] // nh
    wid = residual.shape[1]
    local = residual.shape[0]
    sds = jax.ShapeDtypeStruct

    q, kv = pl.pallas_call(
        functools.partial(pack_kernel, nh),
        out_shape=(sds((nh, rows, 2 * hd), BF), sds((nh, rows, 2 * hd + vd), BF)),
        in_specs=[VM] * 5,
        out_specs=(VM, VM),
        name="pack",
    )(query_one, key_one, query_two, key_two, value_rows)

    g, u, dn = gate_weight[0], up_weight[0], down_weight[0]
    nf = nh * (np_ - 1)
    q_all, kv_all, g2, u2, dn2 = pl.pallas_call(
        functools.partial(gather_kernel, n, nh),
        out_shape=(
            sds((nh, rows, 2 * hd), BF), sds((n, rows, 2 * hd + vd), BF),
            sds(g.shape, BF), sds(u.shape, BF), sds(dn.shape, BF),
        ),
        in_specs=[VM, VM, ANY, ANY, ANY],
        out_specs=(VM, VM, ANY, ANY, ANY),
        scratch_shapes=[
            DMA((nh,)), DMA((nh,)), DMA((nh,)), DMA((nh,)), DMA((nf,)), DMA((nf,)),
            DMA((3,)), DMA((3,)), DMA((2,)),
        ],
        compiler_params=pltpu.CompilerParams(collective_id=1, has_side_effects=True),
        name="gather_heads",
    )(q, kv, g, u, dn)

    attended = pl.pallas_call(
        functools.partial(attention_kernel, np_),
        out_shape=sds((nh, rows, vd), BF),
        grid=(nh,),
        in_specs=[
            pl.BlockSpec((1, rows, 2 * hd), lambda i: (i, 0, 0)),
            VM,
            pl.BlockSpec(memory_space=pltpu.SMEM),
            VM,
        ],
        out_specs=pl.BlockSpec((1, rows, vd), lambda i: (i, 0, 0)),
        scratch_shapes=[
            pltpu.VMEM((n, 2 * rows, rows), F32),
            pltpu.VMEM((2 * rows, min(rows, 128)), F32),
            pltpu.VMEM((2 * rows, 2 * vd), F32),
        ],
        name="attend",
    )(q_all, kv_all, lambda_head, head_gain.reshape(1, vd))

    na = nh * nt - 1
    all_heads = pl.pallas_call(
        functools.partial(heads_kernel, n, nt, nh),
        out_shape=sds((rows // nt, nh * nt * vd), BF),
        in_specs=[VM],
        out_specs=VM,
        scratch_shapes=[DMA((na,)), DMA((na,)), DMA],
        compiler_params=pltpu.CompilerParams(collective_id=2, has_side_effects=True),
        name="return_heads",
    )(attended)

    ne = gate_weight.shape[0] * n
    cap = max(2, (3 * rows + 2 * n - 1) // (2 * n))
    capp = (cap + 7) // 8 * 8
    slots = ne * capp
    after, d0, d1, outgoing = pl.pallas_call(
        functools.partial(route_kernel, ne, cap, capp),
        out_shape=(
            sds((local, wid), BF), sds((local, slots), BF), sds((local, slots), BF), sds((slots, wid), BF),
        ),
        in_specs=[VM] * 5,
        out_specs=(VM, VM, VM, VM),
        name="project_route",
    )(all_heads, out_weight, residual, norm_gain.reshape(1, wid), route_ids)

    ff = g.shape[1]
    block = (n, capp, wid)
    return pl.pallas_call(
        functools.partial(moe_kernel, n, nh),
        out_shape=sds((local, wid), BF),
        in_specs=[ANY] * 7 + [VM] * 4,
        out_specs=VM,
        scratch_shapes=[
            pltpu.VMEM(block, BF), pltpu.VMEM(block, BF), pltpu.VMEM(block, BF),
            pltpu.VMEM((2, wid, ff), BF), pltpu.VMEM((2, wid, ff), BF), pltpu.VMEM((2, ff, wid), BF),
            DMA((n,)), DMA((n,)), DMA((n,)), DMA((n,)), DMA((2,)), DMA((6,)),
        ],
        compiler_params=pltpu.CompilerParams(collective_id=3, has_side_effects=True),
        name="experts",
    )(outgoing.reshape(block), g, u, dn, g2, u2, dn2, d0, d1, route_weights, after)


def solution(mesh):
    placed = (
        P(("sp", "tp"), None), P("sp", "tp"), P("sp", "tp"), P("sp", "tp"), P("sp", "tp"),
        P("sp", "tp"), P("tp"), P(), P(), P(), P(("sp", "tp"), None), P(("sp", "tp"), None),
        P("sp", None, "tp"), P("sp", None, "tp"), P("sp", "tp", None),
    )
    return jax.shard_map(
        on_device, mesh=mesh, in_specs=placed, out_specs=P(("sp", "tp"), None), check_vma=False
    )
```
